256 devices in a mesh: grp: 2 (over y), sp: 32 (over z, core), tp: 4 (over x).
Axes of the slice: x: 4, y: 2, z: 16, core: 2. Of those that a mesh axis runs over, the one named last changes fastest.
The devices are a block of a 4x16x16 slice.
Arguments:
- hidden_in: bfloat16 [16384, 2048], P(('grp', 'sp')), parts along dimension 0, may hold values from -6 to 6
- query_latent_rows: bfloat16 [16384, 768], P(('grp', 'sp')), parts along dimension 0, may hold values from -6 to 6
- key_value_latent: bfloat16 [16384, 512], P(('grp', 'sp')), parts along dimension 0, may hold values from -6 to 6
- rotary_key: bfloat16 [16384, 32], P(('grp', 'sp')), parts along dimension 0, may hold values from -64 to 64
- query_norm_gain: float32 [768], replicated, may hold values from 0.1 to 1.9
- key_value_gain: float32 [512], replicated, may hold values from 0.1 to 1.9
- query_up_weight: bfloat16 [768, 1536], P(None, 'tp'), may hold values from -0.625 to 0.625
- key_value_up_weight: bfloat16 [512, 2048], P(None, 'tp'), may hold values from -0.25 to 0.25
- out_proj: bfloat16 [1024, 2048], P('tp'), may hold values from -0.1875 to 0.1875
- feed_gain: float32 [2048], replicated, may hold values from 0.1 to 1.9
- feed_up: bfloat16 [2048, 8192], P('sp', 'tp'), may hold values from -0.125 to 0.125
- feed_down: bfloat16 [8192, 2048], P('tp', 'sp'), may hold values from -0.0625 to 0.0625
Outputs:
- layer_out: bfloat16 [16384, 2048], P(('grp', 'sp', 'tp')), parts along dimension 0
The draws below stay inside these ranges and needn't reach their ends.
There are 2 independent parts, one for each index of `grp`. The reference program is written for one: setup_inputs(seed, part) draws one part's arguments, and reference() takes and returns one part's arrays. A program takes and returns all parts, laid end to end along the dimension named above; an argument that names none is the same for every part. Nothing has to cross between parts.
All inputs are finite; a program needn't handle non-finite values.
Results may differ from the reference program's by a relative error of at most 0.02.
Values may be sent and summed in bfloat16 or wider, within the bound.
No kernel may reach another device: no remote copies, remote signals or barrier semaphores. Data moves between devices by JAX's collectives and lax.ppermute only.
A program may use at most 128 MiB of HBM per device.

```python
import math
import jax
import jax.numpy as jnp
from jax import lax

D = 2048
HEAD_COUNT = 16
QUERY_KEY_PLAIN = 64
QUERY_KEY_ROTARY = 32
VALUE_HEAD_SIZE = 64
QUERY_RANK = 768
KEY_VALUE_RANK = 512
FF = 8192
TOKEN_COUNT = 8192


def draw_rotary_key(key, part):
    base = jax.random.normal(jax.random.fold_in(key, 11), (TOKEN_COUNT, QUERY_KEY_ROTARY), jnp.float32)
    return jnp.clip(base, -64.0, 64.0).astype(jnp.bfloat16)


def levels(stream_key, shape, shards, smallest, largest):
    level = 1.0
    for axis_at, blocks in shards:
        heights = jax.random.uniform(jax.random.fold_in(jax.random.fold_in(stream_key, 6), axis_at), (blocks,), jnp.float32, smallest / len(shards), largest / len(shards))
        level = level * jnp.repeat(jnp.exp(heights), shape[axis_at] // blocks).reshape((-1,) + (1,) * (len(shape) - 1 - axis_at))
    return level


def centred(stream_key, extent, deviation, limit, shards=(), kind=jnp.bfloat16):
    factor_of = levels(stream_key, extent, shards, -0.22, 0.18) if shards else 1.0
    drawn = jax.random.normal(stream_key, extent, jnp.float32) * deviation * factor_of
    return jnp.minimum(jnp.maximum(drawn, -limit), limit).astype(kind)


def setup_inputs(seed: int = 0, part: int = 0) -> dict:
    streams_of = jax.random.split(jax.random.key(seed), 13)
    part_keys = jax.random.split(jax.random.fold_in(streams_of[12], part), 13)
    hidden_in = centred(part_keys[0], (TOKEN_COUNT, D), 1.0, 6.0, ((0, 32),))
    query_latent_rows = centred(part_keys[1], (TOKEN_COUNT, QUERY_RANK), 1.0, 6.0, ((0, 32),))
    key_value_latent = centred(part_keys[2], (TOKEN_COUNT, KEY_VALUE_RANK), 1.0, 6.0, ((0, 32),))
    rotary_key = draw_rotary_key(jax.random.fold_in(jax.random.fold_in(streams_of[12], part), 71), part)
    query_norm_gain = jnp.clip(1.0 + 0.18 * jax.random.normal(streams_of[4], (QUERY_RANK,), jnp.float32), 0.1, 1.9)
    key_value_gain = jnp.clip(1.0 + 0.18 * jax.random.normal(streams_of[5], (KEY_VALUE_RANK,), jnp.float32), 0.1, 1.9)
    query_up_weight = centred(streams_of[6], (QUERY_RANK, HEAD_COUNT * (QUERY_KEY_PLAIN + QUERY_KEY_ROTARY)), (3 * QUERY_RANK ** -0.5), 0.625, ((1, 4),))
    key_value_up_weight = centred(streams_of[7], (KEY_VALUE_RANK, HEAD_COUNT * (QUERY_KEY_PLAIN + VALUE_HEAD_SIZE)), KEY_VALUE_RANK ** -0.5, 0.25, ((1, 4),))
    out_proj = centred(streams_of[8], (HEAD_COUNT * VALUE_HEAD_SIZE, D), (HEAD_COUNT * VALUE_HEAD_SIZE) ** -0.5, 0.1875, ((0, 4),))
    feed_gain = jnp.clip(1.0 + 0.18 * jax.random.normal(streams_of[9], (D,), jnp.float32), 0.1, 1.9)
    feed_up = centred(streams_of[10], (D, FF), D ** -0.5, 0.125, ((0, 32), (1, 4)))
    feed_down = centred(streams_of[11], (FF, D), FF ** -0.5, 0.0625, ((0, 4), (1, 32)))
    return {"hidden_in": hidden_in, "query_latent_rows": query_latent_rows, "key_value_latent": key_value_latent, "rotary_key": rotary_key, "query_norm_gain": query_norm_gain, "key_value_gain": key_value_gain, "query_up_weight": query_up_weight, "key_value_up_weight": key_value_up_weight, "out_proj": out_proj, "feed_gain": feed_gain, "feed_up": feed_up, "feed_down": feed_down}


def normalize(values, gain):
    floats = values.astype(jnp.float32)
    return floats * lax.rsqrt(lax.optimization_barrier(jnp.mean(floats * floats, axis=-1, keepdims=True)) + 1e-06) * gain.astype(jnp.float32)

def rotate(values, position):
    half_size = values.shape[-1] // 2
    inverse = 10000.0 ** (-jnp.arange(half_size, dtype=jnp.float32) * 2.0 / values.shape[-1])
    angles = position[:, None] * inverse[None, :]
    cosine = jnp.concatenate([jnp.cos(angles), jnp.cos(angles)], axis=-1)
    sine = jnp.concatenate([jnp.sin(angles), jnp.sin(angles)], axis=-1)
    shape = (values.shape[0],) + (1,) * (values.ndim - 2) + (values.shape[-1],)
    turned = jnp.concatenate([-values[..., half_size:], values[..., :half_size]], axis=-1)
    return values * cosine.reshape(shape) + turned * sine.reshape(shape)

def reference(hidden_in, query_latent_rows, key_value_latent, rotary_key, query_norm_gain, key_value_gain, query_up_weight, key_value_up_weight, out_proj, feed_gain, feed_up, feed_down):
    position = jnp.arange(TOKEN_COUNT).astype(jnp.float32)
    scale_factor = (QUERY_KEY_PLAIN + QUERY_KEY_ROTARY) ** (-0.5)
    query_norm = normalize(query_latent_rows, query_norm_gain).astype(jnp.bfloat16)
    queries = jnp.dot(query_norm, query_up_weight, preferred_element_type=jnp.float32).reshape(TOKEN_COUNT, HEAD_COUNT, QUERY_KEY_PLAIN + QUERY_KEY_ROTARY)
    queries = jnp.concatenate([queries[..., :QUERY_KEY_PLAIN], rotate(queries[..., QUERY_KEY_PLAIN:], position)], axis=-1).astype(jnp.bfloat16)
    latent = normalize(key_value_latent, key_value_gain).astype(jnp.bfloat16)
    keys_values = jnp.dot(latent, key_value_up_weight, preferred_element_type=jnp.float32).astype(jnp.bfloat16)
    keys_values = keys_values.reshape(TOKEN_COUNT, HEAD_COUNT, QUERY_KEY_PLAIN + VALUE_HEAD_SIZE)
    key_nope = keys_values[..., :QUERY_KEY_PLAIN].astype(jnp.float32)
    value_rows = keys_values[..., QUERY_KEY_PLAIN:].astype(jnp.float32)
    key_rope = rotate(rotary_key.astype(jnp.float32), position).astype(jnp.bfloat16).astype(jnp.float32)
    block = math.gcd(TOKEN_COUNT, 512)
    query_blocks = queries.reshape(TOKEN_COUNT // block, block, HEAD_COUNT, QUERY_KEY_PLAIN + QUERY_KEY_ROTARY)

    def attend(query_block):
        plain = query_block[..., :QUERY_KEY_PLAIN].astype(jnp.float32)
        turned = query_block[..., QUERY_KEY_PLAIN:].astype(jnp.float32)
        scores = jnp.einsum('qhd,khd->hqk', plain, key_nope) + jnp.einsum('qhd,kd->hqk', turned, key_rope)
        scores = scores * scale_factor
        expo = jnp.exp(scores - lax.optimization_barrier(jnp.max(scores, axis=-1, keepdims=True)))
        total = lax.optimization_barrier(jnp.sum(expo, axis=-1))
        weights = expo.astype(jnp.bfloat16).astype(jnp.float32)
        summed = jnp.einsum('hqk,khd->qhd', weights, value_rows)
        return summed / jnp.transpose(total)[:, :, None]
    mixed = lax.map(attend, query_blocks).reshape(TOKEN_COUNT, HEAD_COUNT * VALUE_HEAD_SIZE).astype(jnp.bfloat16)
    branch = jnp.dot(mixed, out_proj, preferred_element_type=jnp.float32)
    middle = (hidden_in.astype(jnp.float32) + branch).astype(jnp.bfloat16)
    normed = normalize(middle, feed_gain).astype(jnp.bfloat16)
    upward = jnp.dot(normed, feed_up, preferred_element_type=jnp.float32)
    activated = jnp.square(jax.nn.relu(upward)).astype(jnp.bfloat16)
    feed = jnp.dot(activated, feed_down, preferred_element_type=jnp.float32)
    return (middle.astype(jnp.float32) + feed).astype(jnp.bfloat16)
```

```python
import math

import jax
import jax.numpy as jnp
from jax import lax
from jax.experimental import pallas as pl
from jax.experimental.pallas import tpu as pltpu
from jax.sharding import PartitionSpec as P

PLAIN = 64
ROTARY = 32
VALUE = 64
CORES = 2
EPS = 1e-06


def normalize(values, gain):
    floats = values.astype(jnp.float32)
    return floats * lax.rsqrt(jnp.mean(floats * floats, axis=-1, keepdims=True) + EPS) * gain


def kv_body(latent_ref, gain_ref, weight_ref, rope_ref, cos_ref, sin_ref, out_ref):
    tokens = latent_ref.shape[0]
    half = ROTARY // 2
    latent = normalize(latent_ref[...], gain_ref[...]).astype(jnp.bfloat16)
    out_ref[:tokens, :] = jnp.dot(
        latent, weight_ref[...], preferred_element_type=jnp.float32
    ).astype(jnp.bfloat16)
    first, second = rope_ref[:half, :], rope_ref[half:, :]
    cos, sin = cos_ref[...], sin_ref[...]
    turned = jnp.concatenate([first * cos - second * sin, second * cos + first * sin], axis=1)
    out_ref[tokens:, :] = turned.astype(jnp.bfloat16)


def query_body(latent_ref, gain_ref, weight_ref, cos_ref, sin_ref, out_ref):
    half = ROTARY // 2
    size = PLAIN + ROTARY
    query_norm = normalize(latent_ref[...], gain_ref[...]).astype(jnp.bfloat16)
    queries = jnp.dot(query_norm, weight_ref[...], preferred_element_type=jnp.float32).T
    factor = size ** (-0.5) * math.log2(math.e)
    cos, sin = cos_ref[...], sin_ref[...]
    for head in range(queries.shape[0] // size):
        at = head * size
        first = queries[at + PLAIN : at + PLAIN + half]
        second = queries[at + PLAIN + half : at + size]
        rows = jnp.concatenate(
            [queries[at : at + PLAIN], first * cos - second * sin, second * cos + first * sin],
            axis=0,
        )
        out_ref[at : at + size, :] = (rows * factor).astype(jnp.bfloat16)


def attend_body(count, begins, *refs):
    pieces, query_ref = refs[:count], refs[count]
    state_ref = None if begins else refs[count + 1]
    out_ref = refs[-1]
    heads = query_ref.shape[0]
    tokens = pieces[0].shape[0] - ROTARY // 2
    ropes, turned_values = [], []
    for piece in pieces:
        low = piece[tokens:, :]
        rope = jnp.concatenate([low[:, :tokens], low[:, tokens:]], axis=0).astype(jnp.float32)
        rope = jnp.concatenate([rope, jnp.zeros((128 - ROTARY, tokens), jnp.float32)], axis=0)
        ropes.append(rope.T.astype(jnp.bfloat16))
        turned_values.append(piece[:tokens, :].T)
    ones = jnp.ones((16, tokens), jnp.bfloat16)
    for head in range(heads):
        at = head * (PLAIN + VALUE)
        scores = []
        for piece, rope in zip(pieces, ropes):
            left = jnp.concatenate([piece[:tokens, at : at + PLAIN + VALUE], rope], axis=1)
            scores.append(
                jnp.dot(left, query_ref[head], preferred_element_type=jnp.float32)
            )
        top = jnp.max(scores[0], axis=0, keepdims=True)
        for one in scores[1:]:
            top = jnp.maximum(top, jnp.max(one, axis=0, keepdims=True))
        if begins:
            total = None
        else:
            before = state_ref[head, VALUE + 8 : VALUE + 9, :]
            top = jnp.maximum(top, before)
            total = state_ref[head, : VALUE + 16, :] * jnp.exp2(before - top)
        for one, values in zip(scores, turned_values):
            weights = jnp.exp2(one - top).astype(jnp.bfloat16)
            left = jnp.concatenate([values[at + PLAIN : at + PLAIN + VALUE], ones], axis=0)
            update = jnp.dot(left, weights, preferred_element_type=jnp.float32)
            total = update if total is None else total + update
        out_ref[head, : VALUE + 8, :] = total[: VALUE + 8]
        out_ref[head, VALUE + 8 :, :] = jnp.broadcast_to(top, (8, top.shape[1]))


def attend(pieces, queries, state):
    heads, _, columns = queries.shape
    begins = state is None
    operands = (*pieces, queries) + (() if begins else (state,))
    keys = sum(piece.shape[0] - ROTARY // 2 for piece in pieces)
    return pl.pallas_call(
        lambda *refs: attend_body(len(pieces), begins, *refs),
        out_shape=jax.ShapeDtypeStruct((heads, VALUE + 16, columns), jnp.float32),
        cost_estimate=pl.CostEstimate(
            flops=2 * heads * keys * columns * (256 + 128),
            bytes_accessed=2 * keys * 512,
            transcendentals=heads * keys * columns,
        ),
        name="attend",
    )(*operands)


def feed_body(normed_ref, weight_ref, out_ref, sum_ref, act_ref):
    step = pl.program_id(0)
    half = pl.num_programs(0) // 2
    blocks, _, rows, width = weight_ref.shape
    weight = weight_ref[...].reshape(blocks * rows, width)

    @pl.when(step < half)
    def _():
        part = jnp.dot(normed_ref[...], weight, preferred_element_type=jnp.float32)

        @pl.when(step == 0)
        def _():
            sum_ref[...] = part

        @pl.when(jnp.logical_and(step > 0, step < half - 1))
        def _():
            sum_ref[...] += part

        @pl.when(step == half - 1)
        def _():
            act_ref[...] = jnp.square(jnp.maximum(sum_ref[...] + part, 0.0)).astype(jnp.bfloat16)

    @pl.when(step >= half)
    def _():
        out_ref[...] = lax.dot_general(
            act_ref[...], weight, (((1,), (1,)), ((), ())), preferred_element_type=jnp.float32
        ).astype(jnp.bfloat16)


def feed(normed, gathered, shares):
    tokens, width = normed.shape
    hidden = gathered.shape[1]
    rows = gathered.shape[0] // (2 * shares)
    stacked = gathered.reshape(shares, 2, rows, hidden)
    half = 4
    group = shares // half
    return pl.pallas_call(
        feed_body,
        grid=(2 * half,),
        in_specs=[
            pl.BlockSpec((tokens, group * rows), lambda i: (0, jnp.minimum(i, half - 1))),
            pl.BlockSpec((group, 1, rows, hidden), lambda i: (i % half, i // half, 0, 0)),
        ],
        out_specs=pl.BlockSpec((tokens, group * rows), lambda i: (0, jnp.maximum(i - half, 0))),
        out_shape=jax.ShapeDtypeStruct((tokens, width), jnp.bfloat16),
        scratch_shapes=[
            pltpu.VMEM((tokens, hidden), jnp.float32),
            pltpu.VMEM((tokens, hidden), jnp.bfloat16),
        ],
        cost_estimate=pl.CostEstimate(
            flops=4 * tokens * width * hidden,
            bytes_accessed=4 * width * hidden,
            transcendentals=0,
        ),
        name="feed",
    )(normed, stacked)


def swap_sum(value, axis):
    count = lax.axis_size(axis)
    pieces = lax.all_to_all(
        value.reshape(count, -1, value.shape[-1]), axis, 0, 0, tiled=True
    )
    return jnp.sum(pieces.astype(jnp.float32), axis=0)


def from_everyone(value, axis):
    copies = jnp.broadcast_to(value, (lax.axis_size(axis), *value.shape))
    return lax.all_to_all(copies, axis, split_axis=0, concat_axis=0, tiled=True)


def on_device(
    hidden_in,
    query_latent_rows,
    key_value_latent,
    rotary_key,
    query_norm_gain,
    key_value_gain,
    query_up_weight,
    key_value_up_weight,
    out_proj,
    feed_gain,
    feed_up,
    feed_down,
):
    tokens = hidden_in.shape[0]
    shares = lax.axis_size("sp")
    heads = query_up_weight.shape[1] // (PLAIN + ROTARY)
    kv_width = key_value_up_weight.shape[1]
    half = ROTARY // 2

    weights = lax.all_gather(
        jnp.concatenate([feed_up, feed_down.T], axis=0), "sp", axis=0, tiled=True
    )

    position = (lax.axis_index("sp") * tokens + jnp.arange(tokens)).astype(jnp.float32)
    inverse = 10000.0 ** (-jnp.arange(half, dtype=jnp.float32) * 2.0 / ROTARY)
    angles = inverse[:, None] * position[None, :]
    cos, sin = jnp.cos(angles), jnp.sin(angles)

    own = pl.pallas_call(
        kv_body,
        out_shape=jax.ShapeDtypeStruct((tokens + half, kv_width), jnp.bfloat16),
        name="keys_values",
    )(
        key_value_latent,
        key_value_gain.reshape(1, -1),
        key_value_up_weight,
        rotary_key.astype(jnp.float32).T,
        cos,
        sin,
    )
    query_rows = pl.pallas_call(
        query_body,
        out_shape=jax.ShapeDtypeStruct((heads * (PLAIN + ROTARY), tokens), jnp.bfloat16),
        name="queries",
    )(query_latent_rows, query_norm_gain.reshape(1, -1), query_up_weight, cos, sin)

    partner = [(i, i ^ 1) for i in range(shares)]
    upward = [(i, (i + CORES) % shares) for i in range(shares)]
    downward = [(j, i) for i, j in upward]
    other_rows = lax.ppermute(query_rows, "sp", partner)
    both = jnp.concatenate([query_rows, other_rows], axis=1).reshape(
        heads, PLAIN + ROTARY, 2 * tokens
    )
    columns = 2 * tokens
    queries = jnp.concatenate(
        [
            both[:, :PLAIN],
            jnp.zeros((heads, VALUE, columns), jnp.bfloat16),
            both[:, PLAIN:],
            jnp.zeros((heads, 128 - ROTARY, columns), jnp.bfloat16),
        ],
        axis=1,
    )

    ring = shares // CORES
    up, down = own, own
    pieces = [own]
    state = None
    for step in range(ring // 2 + 1):
        with jax.named_scope(f"ring_{step}"):
            arriving = []
            if step < ring // 2:
                up = lax.ppermute(up, "sp", upward)
                arriving.append(up)
            if step < (ring - 1) // 2:
                down = lax.ppermute(down, "sp", downward)
                arriving.append(down)
            state = attend(pieces, queries, state)
            pieces = arriving

    theirs = lax.ppermute(state[:, :, tokens:], "sp", partner)
    mine = state[:, :, :tokens]
    at_top = VALUE + 8
    top = jnp.maximum(mine[:, at_top : at_top + 1], theirs[:, at_top : at_top + 1])
    mine = mine[:, : VALUE + 1] * jnp.exp2(mine[:, at_top : at_top + 1] - top)
    theirs = theirs[:, : VALUE + 1] * jnp.exp2(theirs[:, at_top : at_top + 1] - top)
    summed = mine + theirs
    mixed = (summed[:, :VALUE] / summed[:, VALUE:]).astype(jnp.bfloat16)
    mixed = mixed.reshape(heads * VALUE, tokens)

    share = tokens // lax.axis_size("tp")
    lead = lax.axis_index("tp") * share
    branch = swap_sum(
        lax.dot_general(
            mixed, out_proj, (((0,), (0,)), ((), ())), preferred_element_type=jnp.float32
        ).astype(jnp.bfloat16),
        "tp",
    )
    own_rows = lax.dynamic_slice_in_dim(hidden_in, lead, share, 0)
    middle = (own_rows.astype(jnp.float32) + branch).astype(jnp.bfloat16)
    normed = from_everyone(normalize(middle, feed_gain).astype(jnp.bfloat16), "tp")
    normed = normed.reshape(tokens, -1)
    result = swap_sum(feed(normed, weights, shares), "tp")
    return (middle.astype(jnp.float32) + result).astype(jnp.bfloat16)


def solution(mesh):
    return jax.shard_map(
        on_device,
        mesh=mesh,
        in_specs=(
            P(("grp", "sp"), None),
            P(("grp", "sp"), None),
            P(("grp", "sp"), None),
            P(("grp", "sp"), None),
            P(),
            P(),
            P(None, "tp"),
            P(None, "tp"),
            P("tp", None),
            P(),
            P("sp", "tp"),
            P("tp", "sp"),
        ),
        out_specs=P(("grp", "sp", "tp"), None),
        check_vma=False,
    )
```

```python
import math

import jax
import jax.numpy as jnp
from jax import lax
from jax.experimental import pallas as pl
from jax.experimental.pallas import tpu as pltpu
from jax.sharding import PartitionSpec as P

PLAIN = 64
ROTARY = 32
VALUE = 64
CORES = 2
SHARES = 4
GROUP = 4
EPS = 1e-06
SMEM_SPEC = pl.BlockSpec(memory_space=pltpu.SMEM)
VMEM_SPEC = pl.BlockSpec(memory_space=pltpu.VMEM)


def normalize(values, gain):
    floats = values.astype(jnp.float32)
    return floats * lax.rsqrt(jnp.mean(floats * floats, axis=-1, keepdims=True) + EPS) * gain


def pack_body(rows, index_ref, latent_ref, gain_ref, rope_ref, cos_ref, sin_ref, out_ref, turned_ref):
    half = ROTARY // 2
    shares = latent_ref.shape[0] // rows
    index = index_ref[0]
    mine = latent_ref[pl.ds(pl.multiple_of(index * rows, rows), rows), :]
    out_ref[:rows, :] = normalize(mine, gain_ref[...]).astype(jnp.bfloat16)
    rope = rope_ref[...].astype(jnp.float32).T
    first, second = rope[:half], rope[half:]
    cos, sin = cos_ref[...], sin_ref[...]
    turned_ref[:half, :] = first * cos - second * sin
    turned_ref[half:, :] = second * cos + first * sin
    part = ROTARY // shares
    own = turned_ref[pl.ds(pl.multiple_of(index * part, part), part), :]
    low = jnp.concatenate([own[: part // 2], own[part // 2 :]], axis=1)
    out_ref[rows:, :] = low.astype(jnp.bfloat16)


def query_body(latent_ref, gain_ref, weight_ref, cos_ref, sin_ref, out_ref):
    half = ROTARY // 2
    size = PLAIN + ROTARY
    query_norm = normalize(latent_ref[...], gain_ref[...]).astype(jnp.bfloat16)
    queries = jnp.dot(query_norm, weight_ref[...], preferred_element_type=jnp.float32).T
    factor = size ** (-0.5) * math.log2(math.e)
    cos, sin = cos_ref[...], sin_ref[...]
    for head in range(queries.shape[0] // size):
        at = head * size
        first = queries[at + PLAIN : at + PLAIN + half]
        second = queries[at + PLAIN + half : at + size]
        rows = jnp.concatenate(
            [queries[at : at + PLAIN], first * cos - second * sin, second * cos + first * sin],
            axis=0,
        )
        out_ref[at : at + size, :] = (rows * factor).astype(jnp.bfloat16)


def place(index, steps):
    return lax.rem(index + SHARES - steps, SHARES)


def spread_body(index_ref, own_ref, other_ref, out_ref, rope_ref):
    tokens = own_ref.shape[1]
    size = PLAIN + ROTARY
    part = ROTARY // SHARES
    index = index_ref[0]
    for side, rows_ref in enumerate((own_ref, other_ref)):
        at = slice(tokens * side, tokens * (side + 1))
        blank = jnp.zeros((PLAIN, tokens), jnp.bfloat16)
        for head in range(out_ref.shape[0]):
            plain = rows_ref[size * head : size * head + PLAIN, :]
            pair = (plain, blank) if head % 2 == 0 else (blank, plain)
            out_ref[head, : 2 * PLAIN, at] = jnp.concatenate(pair, axis=0)
            rope_ref[...] = rows_ref[size * head + PLAIN : size * (head + 1), :].astype(jnp.float32)
            blocks = []
            for steps in range(SHARES):
                first = pl.multiple_of(place(index, steps) * part, part)
                block = rope_ref[pl.ds(first, part), :]
                for half in (block[: part // 2], block[part // 2 :]):
                    blocks.extend([half] * GROUP)
            out_ref[head, 2 * PLAIN :, at] = jnp.concatenate(blocks, axis=0).astype(jnp.bfloat16)


def attend_body(begins, *refs):
    count = SHARES
    index, bundles = refs[0][0], refs[1 : count + 1]
    key_weight_ref, value_weight_ref, query_ref = refs[count + 1 : count + 4]
    state_ref = None if begins else refs[count + 4]
    out_ref, rope_ref, key_ref, value_ref = refs[-4:]
    heads, _, columns = query_ref.shape
    width = bundles[0].shape[1]
    tokens = width // 2
    rows = tokens // count
    keys = key_ref.shape[0]
    group = GROUP
    ropes = jnp.concatenate(
        [b[rows * group :, tokens * a : tokens * (a + 1)] for b in bundles for a in range(2)], axis=0
    )
    rope_ref[...] = ropes.astype(jnp.float32).T
    ropes = jnp.concatenate(
        [rope_ref[pl.ds(pl.multiple_of(place(index, k) * rows, rows), rows), :] for k in range(count)],
        axis=0,
    )
    lane = lax.broadcasted_iota(jnp.int32, ropes.shape, 1)
    part = ROTARY // count // 2
    owner = lax.rem(lax.div(lane, part), group)
    latent = jnp.concatenate(
        [b[rows * s : rows * (s + 1)] for s in range(group) for b in bundles], axis=0
    )
    plain = heads * PLAIN
    key_ref[:, :plain] = jnp.dot(
        latent, key_weight_ref[...], preferred_element_type=jnp.float32
    ).astype(jnp.bfloat16)
    key_ref[:, plain:] = jnp.concatenate(
        [jnp.where(owner == s, ropes, 0.0).astype(jnp.bfloat16) for s in range(group)], axis=0
    )
    value_ref[...] = lax.dot_general(
        value_weight_ref[...], latent, (((1,), (1,)), ((), ())), preferred_element_type=jnp.float32
    ).astype(jnp.bfloat16)

    def score(head):
        at = 2 * PLAIN * (head // 2)
        left = jnp.concatenate([key_ref[:, at : at + 2 * PLAIN], key_ref[:, plain:]], axis=1)
        return jnp.dot(left, query_ref[head], preferred_element_type=jnp.float32)

    def absorb(head, scores):
        top = jnp.max(scores, axis=0, keepdims=True)
        if not begins:
            before = state_ref[head, VALUE + 8 : VALUE + 9, :]
            top = jnp.maximum(top, before)
        weights = jnp.exp2(scores - top).astype(jnp.bfloat16)
        left = jnp.concatenate(
            [value_ref[VALUE * head : VALUE * (head + 1)], jnp.ones((16, keys), jnp.bfloat16)], axis=0
        )
        total = jnp.dot(left, weights, preferred_element_type=jnp.float32)[: VALUE + 8]
        if not begins:
            total = state_ref[head, : VALUE + 8, :] * jnp.exp2(before - top) + total
        out_ref[head, : VALUE + 8, :] = total
        out_ref[head, VALUE + 8 :, :] = jnp.broadcast_to(top, (8, columns))

    scores = score(0)
    for head in range(heads):
        following = score(head + 1) if head + 1 < heads else None
        absorb(head, scores)
        scores = following


def attend(index, bundles, key_weight, value_weight, queries, state):
    heads, _, columns = queries.shape
    begins = state is None
    operands = (index, *bundles, key_weight, value_weight, queries) + (() if begins else (state,))
    tokens = bundles[0].shape[1] // 2
    keys = GROUP * tokens
    return pl.pallas_call(
        lambda *refs: attend_body(begins, *refs),
        out_shape=jax.ShapeDtypeStruct((heads, VALUE + 16, columns), jnp.float32),
        in_specs=[SMEM_SPEC] + [VMEM_SPEC] * (len(operands) - 1),
        scratch_shapes=[
            pltpu.VMEM((tokens, 128), jnp.float32),
            pltpu.VMEM((keys, heads * PLAIN + 128), jnp.bfloat16),
            pltpu.VMEM((heads * VALUE, keys), jnp.bfloat16),
        ],
        cost_estimate=pl.CostEstimate(
            flops=2 * heads * keys * columns * (256 + 128),
            bytes_accessed=2 * keys * 512,
            transcendentals=heads * keys * columns,
        ),
        name="attend",
    )(*operands)


def feed_body(normed_ref, weight_ref, out_ref, sum_ref, act_ref):
    step = pl.program_id(0)
    half = pl.num_programs(0) // 2
    blocks, _, rows, width = weight_ref.shape
    weight = weight_ref[...].reshape(blocks * rows, width)

    @pl.when(step < half)
    def _():
        part = jnp.dot(normed_ref[...], weight, preferred_element_type=jnp.float32)

        @pl.when(step == 0)
        def _():
            sum_ref[...] = part

        @pl.when(jnp.logical_and(step > 0, step < half - 1))
        def _():
            sum_ref[...] += part

        @pl.when(step == half - 1)
        def _():
            act_ref[...] = jnp.square(jnp.maximum(sum_ref[...] + part, 0.0)).astype(jnp.bfloat16)

    @pl.when(step >= half)
    def _():
        out_ref[...] = lax.dot_general(
            act_ref[...], weight, (((1,), (1,)), ((), ())), preferred_element_type=jnp.float32
        ).astype(jnp.bfloat16)


def feed(normed, gathered, shares):
    tokens, width = normed.shape
    hidden = gathered.shape[1]
    rows = gathered.shape[0] // (2 * shares)
    stacked = gathered.reshape(shares, 2, rows, hidden)
    half = 4
    group = shares // half
    return pl.pallas_call(
        feed_body,
        grid=(2 * half,),
        in_specs=[
            pl.BlockSpec((tokens, group * rows), lambda i: (0, jnp.minimum(i, half - 1))),
            pl.BlockSpec((group, 1, rows, hidden), lambda i: (i % half, i // half, 0, 0)),
        ],
        out_specs=pl.BlockSpec((tokens, group * rows), lambda i: (0, jnp.maximum(i - half, 0))),
        out_shape=jax.ShapeDtypeStruct((tokens, width), jnp.bfloat16),
        scratch_shapes=[
            pltpu.VMEM((tokens, hidden), jnp.float32),
            pltpu.VMEM((tokens, hidden), jnp.bfloat16),
        ],
        cost_estimate=pl.CostEstimate(
            flops=4 * tokens * width * hidden,
            bytes_accessed=4 * width * hidden,
            transcendentals=0,
        ),
        name="feed",
    )(normed, stacked)


def swap_sum(value, axis):
    count = lax.axis_size(axis)
    pieces = lax.all_to_all(
        value.reshape(count, -1, value.shape[-1]), axis, 0, 0, tiled=True
    )
    return jnp.sum(pieces.astype(jnp.float32), axis=0)


def from_everyone(value, axis):
    copies = jnp.broadcast_to(value, (lax.axis_size(axis), *value.shape))
    return lax.all_to_all(copies, axis, split_axis=0, concat_axis=0, tiled=True)


def on_device(
    hidden_in,
    query_latent_rows,
    key_value_latent,
    rotary_key,
    query_norm_gain,
    key_value_gain,
    query_up_weight,
    key_value_up_weight,
    out_proj,
    feed_gain,
    feed_up,
    feed_down,
):
    tokens = hidden_in.shape[0]
    shares = lax.axis_size("sp")
    heads = query_up_weight.shape[1] // (PLAIN + ROTARY)
    latent_width = key_value_up_weight.shape[0]
    half = ROTARY // 2

    weights = lax.all_gather(
        jnp.concatenate([feed_up, feed_down.T], axis=0), "sp", axis=0, tiled=True
    )

    position = (lax.axis_index("sp") * tokens + jnp.arange(tokens)).astype(jnp.float32)
    inverse = 10000.0 ** (-jnp.arange(half, dtype=jnp.float32) * 2.0 / ROTARY)
    angles = inverse[:, None] * position[None, :]
    cos, sin = jnp.cos(angles), jnp.sin(angles)

    rows = tokens // SHARES
    low = ROTARY * rows // latent_width
    index = lax.axis_index("tp").astype(jnp.int32).reshape(1)
    own = pl.pallas_call(
        lambda *refs: pack_body(rows, *refs),
        in_specs=[SMEM_SPEC] + [VMEM_SPEC] * 5,
        out_shape=jax.ShapeDtypeStruct((rows + low, latent_width), jnp.bfloat16),
        scratch_shapes=[pltpu.VMEM((ROTARY, tokens), jnp.float32)],
        name="pack",
    )(
        index,
        key_value_latent,
        key_value_gain.reshape(1, -1),
        rotary_key,
        cos,
        sin,
    )

    def z_shift(value, chips):
        return lax.ppermute(
            value, "sp", [(i, (i + CORES * chips) % shares) for i in range(shares)]
        )

    def x_shift(value, chips):
        return lax.ppermute(value, "tp", [(i, (i + chips) % SHARES) for i in range(SHARES)])

    partner = [(i, i ^ 1) for i in range(shares)]
    stride = shares // CORES // SHARES
    arrived = [own] + [z_shift(own, stride * k) for k in range(1, SHARES)]

    query_rows = pl.pallas_call(
        query_body,
        out_shape=jax.ShapeDtypeStruct((heads * (PLAIN + ROTARY), tokens), jnp.bfloat16),
        name="queries",
    )(query_latent_rows, query_norm_gain.reshape(1, -1), query_up_weight, cos, sin)
    other_rows = lax.ppermute(query_rows, "sp", partner)
    queries = pl.pallas_call(
        spread_body,
        in_specs=[SMEM_SPEC, VMEM_SPEC, VMEM_SPEC],
        out_shape=jax.ShapeDtypeStruct((heads, 2 * PLAIN + 128, 2 * tokens), jnp.bfloat16),
        scratch_shapes=[pltpu.VMEM((ROTARY, tokens), jnp.float32)],
        name="spread",
    )(index, query_rows, other_rows)
    split = key_value_up_weight.reshape(latent_width, heads, PLAIN + VALUE)
    key_weight = split[:, :, :PLAIN].reshape(latent_width, heads * PLAIN)
    value_weight = split[:, :, PLAIN:].reshape(latent_width, heads * VALUE).T

    bundle = jnp.concatenate([one[:rows] for one in arrived] + [one[rows:] for one in arrived], axis=0)
    bundles = [bundle] + [z_shift(bundle, k) for k in (1, -1, 2)]
    exchange = lambda value: [value] + [x_shift(value, k) for k in range(1, SHARES)]
    ready = [exchange(bundles[0]), exchange(bundles[1])]
    state = None
    for step in range(len(bundles)):
        with jax.named_scope(f"chunk_{step}"):
            state = attend(index, ready[step], key_weight, value_weight, queries, state)
            if step + 2 < len(bundles):
                following, state = lax.optimization_barrier((bundles[step + 2], state))
                ready.append(exchange(following))

    theirs = lax.ppermute(state[:, :, tokens:], "sp", partner)
    mine = state[:, :, :tokens]
    at_top = VALUE + 8
    top = jnp.maximum(mine[:, at_top : at_top + 1], theirs[:, at_top : at_top + 1])
    mine = mine[:, : VALUE + 1] * jnp.exp2(mine[:, at_top : at_top + 1] - top)
    theirs = theirs[:, : VALUE + 1] * jnp.exp2(theirs[:, at_top : at_top + 1] - top)
    summed = mine + theirs
    mixed = (summed[:, :VALUE] / summed[:, VALUE:]).astype(jnp.bfloat16)
    mixed = mixed.reshape(heads * VALUE, tokens)

    share = tokens // lax.axis_size("tp")
    lead = lax.axis_index("tp") * share
    branch = swap_sum(
        lax.dot_general(
            mixed, out_proj, (((0,), (0,)), ((), ())), preferred_element_type=jnp.float32
        ).astype(jnp.bfloat16),
        "tp",
    )
    own_rows = lax.dynamic_slice_in_dim(hidden_in, lead, share, 0)
    middle = (own_rows.astype(jnp.float32) + branch).astype(jnp.bfloat16)
    normed = from_everyone(normalize(middle, feed_gain).astype(jnp.bfloat16), "tp")
    normed = normed.reshape(tokens, -1)
    result = swap_sum(feed(normed, weights, shares), "tp")
    return (middle.astype(jnp.float32) + result).astype(jnp.bfloat16)


def solution(mesh):
    return jax.shard_map(
        on_device,
        mesh=mesh,
        in_specs=(
            P(("grp", "sp"), None),
            P(("grp", "sp"), None),
            P(("grp", "sp"), None),
            P(("grp", "sp"), None),
            P(),
            P(),
            P(None, "tp"),
            P(None, "tp"),
            P("tp", None),
            P(),
            P("sp", "tp"),
            P("tp", "sp"),
        ),
        out_specs=P(("grp", "sp", "tp"), None),
        check_vma=False,
    )
```
